32 devices in a mesh: fs: 16 (over z, y, core), tp: 2 (over x).
Axes of the slice: x: 2, y: 2, z: 4, core: 2. Of those that a mesh axis runs over, the one named last changes fastest.
Arguments:
- tokens: bfloat16 [4096, 2048], P('fs', 'tp'), may hold values from -16 to 16, as said below
- mix_gain: bfloat16 [2048], P('tp'), may hold values from 0.099609375 to 1.8984375
- query_weight: bfloat16 [2048, 512], P('fs', 'tp'), may hold values from -0.125 to 0.125
- key_weight: bfloat16 [2048, 512], P('fs', 'tp'), may hold values from -0.125 to 0.125
- value_weight: bfloat16 [2048, 1024], P('fs', 'tp'), may hold values from -0.125 to 0.125
- output_gate_weight: bfloat16 [2048, 1024], P('fs', 'tp'), may hold values from -0.125 to 0.125
- out_weight: bfloat16 [1024, 2048], P('tp', 'fs'), may hold values from -0.1875 to 0.1875
- head_rates: float32 [8], P('tp'), may hold values from 0 to 1, as said below
- block_scale: float32 [32], P('fs'), may hold values from 0.5 to 2
- ffn_gain: bfloat16 [2048], P('tp'), may hold values from 0.099609375 to 1.8984375
- ff_gate: bfloat16 [2048, 5632], P('fs', 'tp'), may hold values from -0.125 to 0.125
- ff_up: bfloat16 [2048, 5632], P('fs', 'tp'), may hold values from -0.125 to 0.125
- ff_down: bfloat16 [5632, 2048], P('tp', 'fs'), may hold values from -0.078125 to 0.078125
- final_gain: bfloat16 [2048], P('tp'), may hold values from 0.099609375 to 1.8984375
Outputs:
- layer_out: bfloat16 [4096, 2048], P('fs', 'tp')
The draws below stay inside these ranges and needn't reach their ends.
Inputs may be any that keep to these rules, and one draw needn't show every extreme that they name: `tokens`: column blocks of the activations have different scales. `head_rates`: positive rates.
All inputs are finite; a program needn't handle non-finite values.
Results may differ from the reference program's by a relative error of at most 0.014.
Values may be sent and summed in bfloat16 or wider, within the bound.
A program may use at most 128 MiB of HBM per device.

```python
import math
import jax
import jax.numpy as jnp
from jax import lax

D = 2048
HEADS = 8
DK = 64
DV = 128
FF = 5632
BLK = 128
SEQ_LEN = 256
TOKENS = 4096
N_TP = 2


def draw_tokens(key, part):
    first, second, third = jax.random.split(jax.random.fold_in(key, 11), 3)
    groups = 2 * N_TP
    scales = jnp.exp(jax.random.uniform(second, (groups,), jnp.float32, -1.2, 1.2))
    base = jnp.clip(jax.random.normal(first, (TOKENS, D), jnp.float32), -4.0, 4.0)
    shaped = base.reshape(TOKENS, groups, D // groups) * scales[None, :, None]
    return shaped.reshape(TOKENS, D).astype(jnp.bfloat16)


def draw_head_rates(key, part):
    first, second, third = jax.random.split(jax.random.fold_in(key, 23), 3)
    fast = jax.random.uniform(first, (HEADS,), jnp.float32, 2.8, 4.3) / BLK
    slow = jax.random.uniform(second, (HEADS,), jnp.float32, 0.3, 1.0) / SEQ_LEN
    order = jax.random.permutation(third, HEADS)
    quick = order < HEADS // 2
    return jnp.where(quick, fast, slow).astype(jnp.float32)


def block_levels(own_key, dims, cuts, low, largest):
    level, own = 1.0, jax.random.fold_in(own_key, 6)
    for dim, parts in cuts:
        heights = jnp.exp(jax.random.uniform(jax.random.fold_in(own, dim), (parts,), jnp.float32, low / len(cuts), largest / len(cuts)))
        level = level * jnp.repeat(heights, dims[dim] // parts).reshape([-1 if axis == dim else 1 for axis in range(len(dims))])
    return level


def noise(rng, extent, scale, limit, shards=(), held_as=jnp.bfloat16):
    drawn = scale * jax.random.normal(rng, extent, jnp.float32)
    if shards:
        drawn = drawn * block_levels(rng, extent, shards, -0.22, 0.18)
    return jnp.clip(drawn, -limit, limit).astype(held_as)


def setup_inputs(seed: int = 0) -> dict:
    seeds = jax.random.split(jax.random.key(seed), 15)
    tokens = draw_tokens(jax.random.fold_in(seeds[14], 71), 0)
    mix_gain = jnp.clip(1.0 + 0.18 * jax.random.normal(seeds[1], (D,), jnp.float32), 0.099609375, 1.8984375).astype(jnp.bfloat16)
    query_weight = noise(seeds[2], (D, HEADS * DK), D ** -0.5, 0.125, ((0, 16), (1, 2)))
    key_weight = noise(seeds[3], (D, HEADS * DK), D ** -0.5, 0.125, ((0, 16), (1, 2)))
    value_weight = noise(seeds[4], (D, HEADS * DV), D ** -0.5, 0.125, ((0, 16), (1, 2)))
    output_gate_weight = noise(seeds[5], (D, HEADS * DV), D ** -0.5, 0.125, ((0, 16), (1, 2)))
    out_weight = noise(seeds[6], (HEADS * DV, D), (HEADS * DV) ** -0.5, 0.1875, ((0, 2), (1, 16)))
    head_rates = draw_head_rates(jax.random.fold_in(seeds[14], 71), 0)
    block_scale = jnp.clip(jnp.exp(math.log(2.0) - 1.3862944 * jax.random.uniform(seeds[8], (TOKENS // BLK,), jnp.float32) ** block_levels(seeds[8], (TOKENS // BLK,), ((0, 16),), -0.2, 0.2)), 0.5, 2.0)
    ffn_gain = jnp.clip(1.0 + 0.18 * jax.random.normal(seeds[9], (D,), jnp.float32), 0.099609375, 1.8984375).astype(jnp.bfloat16)
    ff_gate = noise(seeds[10], (D, FF), D ** -0.5, 0.125, ((0, 16), (1, 2)))
    ff_up = noise(seeds[11], (D, FF), D ** -0.5, 0.125, ((0, 16), (1, 2)))
    ff_down = noise(seeds[12], (FF, D), FF ** -0.5, 0.078125, ((0, 2), (1, 16)))
    final_gain = jnp.clip(1.0 + 0.18 * jax.random.normal(seeds[13], (D,), jnp.float32), 0.099609375, 1.8984375).astype(jnp.bfloat16)
    return dict(tokens=tokens, mix_gain=mix_gain, query_weight=query_weight, key_weight=key_weight, value_weight=value_weight, output_gate_weight=output_gate_weight, out_weight=out_weight, head_rates=head_rates, block_scale=block_scale, ffn_gain=ffn_gain, ff_gate=ff_gate, ff_up=ff_up, ff_down=ff_down, final_gain=final_gain)


EPS = 1e-06
THETA = 10000.0

def rms_norm(values, gain):
    scale = lax.rsqrt(lax.optimization_barrier(jnp.mean(values * values, axis=-1, keepdims=True)) + EPS)
    return values * scale * gain.astype(jnp.float32)

def rotate(values, positions):
    half = values.shape[-1] // 2
    inverse = THETA ** (-jnp.arange(half, dtype=jnp.float32) / half)
    angle = positions.astype(jnp.float32)[:, None] * inverse
    cosine = jnp.cos(angle)[:, None, :]
    sine = jnp.sin(angle)[:, None, :]
    first = values[..., :half]
    second = values[..., half:]
    return jnp.concatenate([first * cosine - second * sine, second * cosine + first * sine], axis=-1)

def retain(query, key, value, rates, scales):
    rows, heads_here, width_k = query.shape
    width_v = value.shape[-1]
    nblk = rows // BLK
    hi = lax.Precision.HIGHEST
    qblk = query.astype(jnp.float32).reshape(nblk, BLK, heads_here, width_k)
    kblk = key.astype(jnp.float32).reshape(nblk, BLK, heads_here, width_k)
    vblk = value.astype(jnp.float32).reshape(nblk, BLK, heads_here, width_v)
    logdec = -rates[None, :] * scales[:, None]
    steps = jnp.arange(BLK, dtype=jnp.float32)
    offset = steps[:, None] - steps[None, :]
    causal = offset >= 0
    inside = jnp.where(causal[None, None], jnp.exp(logdec[:, :, None, None] * jnp.where(causal, offset, 0.0)[None, None]), 0.0)
    scores = jnp.einsum('nchd,nmhd->nhcm', qblk, kblk, precision=hi) * inside
    inner = jnp.einsum('nhcm,nmhe->nche', scores, vblk, precision=hi)
    zeta = jnp.exp(logdec[:, :, None] * (BLK - 1.0 - steps)[None, None, :])
    kv_block = jnp.einsum('nchd,nche->nhde', kblk * jnp.transpose(zeta, (0, 2, 1))[..., None], vblk, precision=hi)
    hold = jnp.exp(logdec * BLK)
    per_seq = SEQ_LEN // BLK
    fresh = (jnp.arange(nblk, dtype=jnp.int32) % per_seq == 0).astype(jnp.float32)

    def advance(state, inputs):
        kv_now, hold_now, fresh_now = inputs
        before = state * (1.0 - fresh_now)
        return (before * hold_now[:, None, None] + kv_now, before)
    start = jnp.zeros((heads_here, width_k, width_v), jnp.float32)
    _, before = lax.scan(advance, start, (kv_block, hold, fresh))
    xi = jnp.exp(logdec[:, :, None] * (steps + 1.0)[None, None, :])
    cross = jnp.einsum('nchd,nhde->nche', qblk * jnp.transpose(xi, (0, 2, 1))[..., None], before, precision=hi)
    total = inner + cross
    total = total * lax.rsqrt(lax.optimization_barrier(jnp.mean(total * total, axis=-1, keepdims=True)) + EPS)
    return total.reshape(rows, heads_here, width_v)

def grouped_product(left, right, groups):
    width = left.shape[1] // groups
    result = jnp.zeros((left.shape[0], right.shape[1]), jnp.float32)
    for index in range(groups):
        partial_sum = jnp.dot(left[:, index * width:(index + 1) * width], right[index * width:(index + 1) * width], preferred_element_type=jnp.float32)
        result = result + partial_sum.astype(jnp.bfloat16).astype(jnp.float32)
    return result

def reference(tokens, mix_gain, query_weight, key_weight, value_weight, output_gate_weight, out_weight, head_rates, block_scale, ffn_gain, ff_gate, ff_up, ff_down, final_gain):
    rows = tokens.shape[0]
    positions = jnp.arange(rows, dtype=jnp.int32) % SEQ_LEN
    normed = rms_norm(tokens.astype(jnp.float32), mix_gain).astype(jnp.bfloat16)
    qproj = jnp.dot(normed, query_weight, preferred_element_type=jnp.float32).reshape(rows, HEADS, DK)
    kproj = jnp.dot(normed, key_weight, preferred_element_type=jnp.float32).reshape(rows, HEADS, DK)
    vproj = jnp.dot(normed, value_weight, preferred_element_type=jnp.float32)
    gproj = jnp.dot(normed, output_gate_weight, preferred_element_type=jnp.float32)
    query = rotate(qproj, positions).astype(jnp.bfloat16)
    key = (rotate(kproj, positions) * DK ** (-0.5)).astype(jnp.bfloat16)
    value = vproj.astype(jnp.bfloat16).reshape(rows, HEADS, DV)
    normret = retain(query, key, value, head_rates, block_scale).reshape(rows, HEADS * DV)
    gated = (normret * jax.nn.silu(gproj)).astype(jnp.bfloat16)
    mix = grouped_product(gated, out_weight, N_TP)
    resid = (tokens.astype(jnp.float32) + mix).astype(jnp.bfloat16)
    normed2 = rms_norm(resid.astype(jnp.float32), ffn_gain).astype(jnp.bfloat16)
    gate_part = jnp.dot(normed2, ff_gate, preferred_element_type=jnp.float32)
    up_part = jnp.dot(normed2, ff_up, preferred_element_type=jnp.float32)
    hidden = (jax.nn.silu(gate_part) * up_part).astype(jnp.bfloat16)
    ffn = grouped_product(hidden, ff_down, N_TP)
    total = resid.astype(jnp.float32) + ffn
    return rms_norm(total, final_gain).astype(jnp.bfloat16)
```

```python
import jax
import jax.numpy as jnp
from jax import lax
from jax.sharding import PartitionSpec as P

D = 2048
DK = 64
DV = 128
BLK = 128
SEQ_LEN = 256


EPS = 1e-06
THETA = 10000.0


def rms_norm(values, gain):
    scale = lax.rsqrt(jnp.mean(values * values, axis=-1, keepdims=True) + EPS)
    return values * scale * gain.astype(jnp.float32)


def rotate(values, positions):
    half = values.shape[-1] // 2
    inverse = THETA ** (-jnp.arange(half, dtype=jnp.float32) / half)
    angle = positions.astype(jnp.float32)[:, None] * inverse
    cosine = jnp.cos(angle)[:, None, :]
    sine = jnp.sin(angle)[:, None, :]
    first = values[..., :half]
    second = values[..., half:]
    return jnp.concatenate(
        [first * cosine - second * sine, second * cosine + first * sine], axis=-1
    )


def retain(query, key, value, rates, scales):
    rows, heads_here, width_k = query.shape
    width_v = value.shape[-1]
    nblk = rows // BLK
    hi = lax.Precision.HIGHEST
    qblk = query.astype(jnp.float32).reshape(nblk, BLK, heads_here, width_k)
    kblk = key.astype(jnp.float32).reshape(nblk, BLK, heads_here, width_k)
    vblk = value.astype(jnp.float32).reshape(nblk, BLK, heads_here, width_v)
    logdec = -rates[None, :] * scales[:, None]
    steps = jnp.arange(BLK, dtype=jnp.float32)
    offset = steps[:, None] - steps[None, :]
    causal = offset >= 0
    inside = jnp.where(
        causal[None, None],
        jnp.exp(logdec[:, :, None, None] * jnp.where(causal, offset, 0.0)[None, None]),
        0.0,
    )
    scores = jnp.einsum("nchd,nmhd->nhcm", qblk, kblk, precision=hi) * inside
    inner = jnp.einsum("nhcm,nmhe->nche", scores, vblk, precision=hi)
    zeta = jnp.exp(logdec[:, :, None] * (BLK - 1.0 - steps)[None, None, :])
    kv_block = jnp.einsum(
        "nchd,nche->nhde", kblk * jnp.transpose(zeta, (0, 2, 1))[..., None], vblk, precision=hi
    )
    hold = jnp.exp(logdec * BLK)
    per_seq = SEQ_LEN // BLK
    fresh = (jnp.arange(nblk, dtype=jnp.int32) % per_seq == 0).astype(jnp.float32)

    def advance(state, inputs):
        kv_now, hold_now, fresh_now = inputs
        before = state * (1.0 - fresh_now)
        return (before * hold_now[:, None, None] + kv_now, before)

    start = jnp.zeros((heads_here, width_k, width_v), jnp.float32)
    _, before = lax.scan(advance, start, (kv_block, hold, fresh))
    xi = jnp.exp(logdec[:, :, None] * (steps + 1.0)[None, None, :])
    cross = jnp.einsum(
        "nchd,nhde->nche", qblk * jnp.transpose(xi, (0, 2, 1))[..., None], before, precision=hi
    )
    total = inner + cross
    total = total * lax.rsqrt(jnp.mean(total * total, axis=-1, keepdims=True) + EPS)
    return total.reshape(rows, heads_here * width_v)


def chip_ring(size):
    chips = size // 2
    return list(range(0, chips, 2)) + list(range(1, chips, 2))[::-1]


def ring_place(size):
    ring = chip_ring(size)
    me = lax.axis_index("fs")
    chip = me // 2
    place = jnp.zeros((), jnp.int32)
    for index, member in enumerate(ring):
        place = jnp.where(chip == member, index, place)
    return place, me % 2


def after(value, *others):
    return lax.optimization_barrier((value,) + tuple(others))[0]


def circulate(block, axis, starts=()):
    size = lax.axis_size("fs")
    ring = chip_ring(size)
    chips = len(ring)
    onward = [
        (2 * ring[i] + core, 2 * ring[(i + 1) % chips] + core)
        for i in range(chips)
        for core in range(2)
    ]
    back = [(target, source) for source, target in onward]
    swap = [(i, i ^ 1) for i in range(size)]
    if starts:
        block = after(block, *starts)
    held = {0: block}
    reach = (chips - 1) // 2
    down = up = block
    for step in range(1, reach + 1):
        down = lax.ppermute(down, "fs", onward)
        up = lax.ppermute(up, "fs", back)
        held[-step] = down
        held[step] = up
    if chips % 2 == 0 and chips > 1:
        cut = 1 - axis
        half = block.shape[cut] // 2
        first = lax.ppermute(lax.slice_in_dim(down, 0, half, axis=cut), "fs", onward)
        second = lax.ppermute(lax.slice_in_dim(up, half, None, axis=cut), "fs", back)
        held[reach + 1] = jnp.concatenate([first, second], axis=cut)
    return {k: (v, lax.ppermute(v, "fs", swap)) for k, v in held.items()}


def order_of(size):
    chips = size // 2
    reach = (chips - 1) // 2
    early = list(range(-(reach - 1), reach)) if reach > 1 else [0]
    first = early[0]
    late = [o if o <= chips // 2 else o - chips for o in range(early[-1] + 1, first + chips)]
    return early, late


def join(blocks, offsets, axis):
    return jnp.concatenate([b for o in offsets for b in blocks[o]], axis=axis)


def pair_swap(values, wide):
    pieces = [values[:, i * wide : (i + 1) * wide] for i in range(values.shape[1] // wide)]
    return jnp.concatenate([pieces[i ^ 1] for i in range(len(pieces))], axis=1)


def to_ring(values, place, core):
    size = lax.axis_size("fs")
    wide = values.shape[1] // size
    ring = chip_ring(size)
    chips = len(ring)
    ringed = jnp.concatenate([values[:, 2 * c * wide : 2 * (c + 1) * wide] for c in ring] * 2, axis=1)
    start = (place + order_of(size)[0][0] + chips) % chips
    rolled = lax.dynamic_slice_in_dim(ringed, start * (2 * wide), chips * 2 * wide, axis=1)
    return jnp.where(core == 0, rolled, pair_swap(rolled, wide))


def from_ring(values, place, core):
    size = lax.axis_size("fs")
    wide = values.shape[1] // size
    ring = chip_ring(size)
    chips = len(ring)
    straight = jnp.where(core == 0, values, pair_swap(values, wide))
    start = (2 * chips - place - order_of(size)[0][0]) % chips
    doubled = jnp.concatenate([straight, straight], axis=1)
    rolled = lax.dynamic_slice_in_dim(doubled, start * (2 * wide), chips * 2 * wide, axis=1)
    spot = {c: i for i, c in enumerate(ring)}
    return jnp.concatenate(
        [rolled[:, 2 * spot[c] * wide : 2 * (spot[c] + 1) * wide] for c in range(chips)], axis=1
    )


def tp_gather(values, axis):
    if lax.axis_size("tp") != 2:
        return lax.all_gather(values, "tp", axis=axis, tiled=True)
    other = lax.ppermute(values, "tp", [(0, 1), (1, 0)])
    mine = lax.axis_index("tp") == 0
    return jnp.concatenate(
        [jnp.where(mine, values, other), jnp.where(mine, other, values)], axis=axis
    )


def tp_scatter_sum(partial):
    if lax.axis_size("tp") != 2:
        pieces = lax.all_to_all(
            partial.reshape(partial.shape[0], lax.axis_size("tp"), -1), "tp", 1, 1
        )
        return jnp.sum(pieces.astype(jnp.float32), axis=1)
    half = partial.shape[1] // 2
    low = lax.axis_index("tp") == 0
    keep = jnp.where(low, partial[:, :half], partial[:, half:])
    send = jnp.where(low, partial[:, half:], partial[:, :half])
    got = lax.ppermute(send, "tp", [(0, 1), (1, 0)])
    return keep.astype(jnp.float32) + got.astype(jnp.float32)


def product_rows(left, blocks):
    early, late = order_of(lax.axis_size("fs"))
    first, second = join(blocks, early, 0), join(blocks, late, 0)
    depth = first.shape[0]
    return jnp.dot(left[:, :depth], first, preferred_element_type=jnp.float32) + jnp.dot(
        left[:, depth:], second, preferred_element_type=jnp.float32
    )


def product_columns(left, blocks, place, core):
    early, late = order_of(lax.axis_size("fs"))
    parts = [
        jnp.dot(left, join(blocks, offsets, 1), preferred_element_type=jnp.float32).astype(
            jnp.bfloat16
        )
        for offsets in (early, late)
    ]
    return from_ring(jnp.concatenate(parts, axis=1), place, core)


def body(
    tokens,
    mix_gain,
    query_weight,
    key_weight,
    value_weight,
    output_gate_weight,
    out_weight,
    head_rates,
    block_scale,
    ffn_gain,
    ff_gate,
    ff_up,
    ff_down,
    final_gain,
):
    rows = tokens.shape[0]
    heads_here = head_rates.shape[0]
    size = lax.axis_size("fs")
    place, core = ring_place(size)
    reach = (size // 2 - 1) // 2
    positions = jnp.arange(rows, dtype=jnp.int32) % SEQ_LEN

    bundle = jnp.concatenate([query_weight, key_weight, value_weight, output_gate_weight], axis=1)
    proj = circulate(bundle, 0)
    out_cols = circulate(out_weight, 1)
    gates = circulate(ff_gate, 0, (proj[-reach][0], proj[reach][0]))
    ups = circulate(ff_up, 0, (proj[-reach][0], proj[reach][0]))
    downs = circulate(ff_down, 1, (gates[-reach][0], gates[reach][0]))

    whole = tp_gather(tokens, 1)
    gains = tp_gather(jnp.stack([mix_gain, ffn_gain]), 1)
    normed = rms_norm(whole.astype(jnp.float32), gains[0]).astype(jnp.bfloat16)
    projected = product_rows(to_ring(normed, place, core), proj)
    ends = [query_weight.shape[1], key_weight.shape[1], value_weight.shape[1]]
    qproj, kproj, vproj, gproj = jnp.split(
        projected, [ends[0], ends[0] + ends[1], sum(ends)], axis=1
    )
    query = rotate(qproj.reshape(rows, heads_here, DK), positions).astype(jnp.bfloat16)
    key = (rotate(kproj.reshape(rows, heads_here, DK), positions) * DK ** (-0.5)).astype(
        jnp.bfloat16
    )
    value = vproj.astype(jnp.bfloat16).reshape(rows, heads_here, DV)
    normret = retain(query, key, value, head_rates, block_scale)
    gated = (normret * jax.nn.silu(gproj)).astype(jnp.bfloat16)
    mix = tp_scatter_sum(product_columns(gated, out_cols, place, core))
    resid = (tokens.astype(jnp.float32) + mix).astype(jnp.bfloat16)
    whole2 = tp_gather(resid, 1)
    normed2 = to_ring(
        rms_norm(whole2.astype(jnp.float32), gains[1]).astype(jnp.bfloat16), place, core
    )
    gate_part = product_rows(normed2, gates)
    up_part = product_rows(normed2, ups)
    hidden = (jax.nn.silu(gate_part) * up_part).astype(jnp.bfloat16)
    ffn = tp_scatter_sum(product_columns(hidden, downs, place, core))
    total = resid.astype(jnp.float32) + ffn
    squares = lax.psum(jnp.sum(total * total, axis=-1, keepdims=True), "tp")
    scale = lax.rsqrt(squares / D + EPS)
    return (total * scale * final_gain.astype(jnp.float32)).astype(jnp.bfloat16)


def solution(mesh):
    return jax.shard_map(
        body,
        mesh=mesh,
        in_specs=(
            P("fs", "tp"),
            P("tp"),
            P("fs", "tp"),
            P("fs", "tp"),
            P("fs", "tp"),
            P("fs", "tp"),
            P("tp", "fs"),
            P("tp"),
            P("fs"),
            P("tp"),
            P("fs", "tp"),
            P("fs", "tp"),
            P("tp", "fs"),
            P("tp"),
        ),
        out_specs=P("fs", "tp"),
        check_vma=False,
    )
```

```python
import jax
import jax.numpy as jnp
from jax import lax
from jax.sharding import PartitionSpec as P

D = 2048
DK = 64
DV = 128
BLK = 128
SEQ_LEN = 256


EPS = 1e-06
THETA = 10000.0


def rms_norm(values, gain):
    scale = lax.rsqrt(jnp.mean(values * values, axis=-1, keepdims=True) + EPS)
    return values * scale * gain.astype(jnp.float32)


def rotate(values, positions):
    half = values.shape[-1] // 2
    inverse = THETA ** (-jnp.arange(half, dtype=jnp.float32) / half)
    angle = positions.astype(jnp.float32)[:, None] * inverse
    cosine = jnp.cos(angle)[:, None, :]
    sine = jnp.sin(angle)[:, None, :]
    first = values[..., :half]
    second = values[..., half:]
    return jnp.concatenate(
        [first * cosine - second * sine, second * cosine + first * sine], axis=-1
    )


def retain(query, key, value, rates, scales):
    rows, heads_here, width_k = query.shape
    width_v = value.shape[-1]
    nblk = rows // BLK
    hi = lax.Precision.HIGHEST
    qblk = query.astype(jnp.float32).reshape(nblk, BLK, heads_here, width_k)
    kblk = key.astype(jnp.float32).reshape(nblk, BLK, heads_here, width_k)
    vblk = value.astype(jnp.float32).reshape(nblk, BLK, heads_here, width_v)
    logdec = -rates[None, :] * scales[:, None]
    steps = jnp.arange(BLK, dtype=jnp.float32)
    offset = steps[:, None] - steps[None, :]
    causal = offset >= 0
    inside = jnp.where(
        causal[None, None],
        jnp.exp(logdec[:, :, None, None] * jnp.where(causal, offset, 0.0)[None, None]),
        0.0,
    )
    scores = jnp.einsum("nchd,nmhd->nhcm", qblk, kblk, precision=hi) * inside
    inner = jnp.einsum("nhcm,nmhe->nche", scores, vblk, precision=hi)
    zeta = jnp.exp(logdec[:, :, None] * (BLK - 1.0 - steps)[None, None, :])
    kv_block = jnp.einsum(
        "nchd,nche->nhde", kblk * jnp.transpose(zeta, (0, 2, 1))[..., None], vblk, precision=hi
    )
    hold = jnp.exp(logdec * BLK)
    per_seq = SEQ_LEN // BLK
    fresh = (jnp.arange(nblk, dtype=jnp.int32) % per_seq == 0).astype(jnp.float32)

    def advance(state, inputs):
        kv_now, hold_now, fresh_now = inputs
        before = state * (1.0 - fresh_now)
        return (before * hold_now[:, None, None] + kv_now, before)

    start = jnp.zeros((heads_here, width_k, width_v), jnp.float32)
    _, before = lax.scan(advance, start, (kv_block, hold, fresh), unroll=True)
    xi = jnp.exp(logdec[:, :, None] * (steps + 1.0)[None, None, :])
    cross = jnp.einsum(
        "nchd,nhde->nche", qblk * jnp.transpose(xi, (0, 2, 1))[..., None], before, precision=hi
    )
    total = inner + cross
    total = total * lax.rsqrt(jnp.mean(total * total, axis=-1, keepdims=True) + EPS)
    return total.reshape(rows, heads_here * width_v)


def chip_ring(size):
    chips = size // 2
    return list(range(0, chips, 2)) + list(range(1, chips, 2))[::-1]


def ring_place(size):
    ring = chip_ring(size)
    me = lax.axis_index("fs")
    chip = me // 2
    place = jnp.zeros((), jnp.int32)
    for index, member in enumerate(ring):
        place = jnp.where(chip == member, index, place)
    return place, me % 2


def after(value, *others):
    return lax.optimization_barrier((value,) + tuple(others))[0]


def circulate(block, axis, gates=()):
    size = lax.axis_size("fs")
    ring = chip_ring(size)
    chips = len(ring)
    onward = [
        (2 * ring[i] + core, 2 * ring[(i + 1) % chips] + core)
        for i in range(chips)
        for core in range(2)
    ]
    back = [(target, source) for source, target in onward]
    swap = [(i, i ^ 1) for i in range(size)]
    held = {0: block}
    reach = (chips - 1) // 2
    down = up = block
    for step in range(1, reach + 1):
        if len(gates) >= step and gates[step - 1]:
            down = after(down, *gates[step - 1])
            up = after(up, *gates[step - 1])
        down = lax.ppermute(down, "fs", onward)
        up = lax.ppermute(up, "fs", back)
        held[-step] = down
        held[step] = up
    if chips % 2 == 0 and chips > 1:
        cut = 1 - axis
        half = block.shape[cut] // 2
        first = lax.ppermute(lax.slice_in_dim(down, 0, half, axis=cut), "fs", onward)
        second = lax.ppermute(lax.slice_in_dim(up, half, None, axis=cut), "fs", back)
        held[reach + 1] = jnp.concatenate([first, second], axis=cut)
    groups = []
    for offsets in order_of(size):
        own = jnp.concatenate([held[o] for o in offsets], axis=axis)
        groups.append((own, lax.ppermute(own, "fs", swap)))
    return held, groups


def order_of(size):
    chips = size // 2
    reach = (chips - 1) // 2
    early = list(range(-(reach - 1), reach)) if reach > 1 else [0]
    first = early[0]
    late = [o if o <= chips // 2 else o - chips for o in range(early[-1] + 1, first + chips)]
    return early, late


def lane_of(values, lane, wide):
    count = values.shape[1] // (2 * wide)
    return [values[:, (2 * c + lane) * wide : (2 * c + lane + 1) * wide] for c in range(count)]


def to_ring(values, place, core):
    size = lax.axis_size("fs")
    wide = values.shape[1] // size
    ring = chip_ring(size)
    chips = len(ring)
    early, late = order_of(size)
    start = (place + early[0] + chips) % chips
    lanes = []
    for lane in range(2):
        pieces = lane_of(values, lane, wide)
        ringed = jnp.concatenate([pieces[c] for c in ring] * 2, axis=1)
        lanes.append(lax.dynamic_slice_in_dim(ringed, start * wide, chips * wide, axis=1))
    own = jnp.where(core == 0, lanes[0], lanes[1])
    other = jnp.where(core == 0, lanes[1], lanes[0])
    edge = len(early) * wide
    return [(own[:, :edge], other[:, :edge]), (own[:, edge:], other[:, edge:])]


def from_ring(groups, place, core):
    size = lax.axis_size("fs")
    ring = chip_ring(size)
    chips = len(ring)
    own = jnp.concatenate([own for own, _ in groups], axis=1)
    other = jnp.concatenate([other for _, other in groups], axis=1)
    wide = own.shape[1] // chips
    start = (2 * chips - place - order_of(size)[0][0]) % chips
    lanes = []
    for lane in range(2):
        straight = jnp.where(core == lane, own, other)
        doubled = jnp.concatenate([straight, straight], axis=1)
        lanes.append(lax.dynamic_slice_in_dim(doubled, start * wide, chips * wide, axis=1))
    spot = {c: i for i, c in enumerate(ring)}
    return jnp.concatenate(
        [
            lanes[lane][:, spot[c] * wide : (spot[c] + 1) * wide]
            for c in range(chips)
            for lane in range(2)
        ],
        axis=1,
    )


def tp_gather(values, axis):
    if lax.axis_size("tp") != 2:
        return lax.all_gather(values, "tp", axis=axis, tiled=True)
    other = lax.ppermute(values, "tp", [(0, 1), (1, 0)])
    mine = lax.axis_index("tp") == 0
    return jnp.concatenate(
        [jnp.where(mine, values, other), jnp.where(mine, other, values)], axis=axis
    )


def tp_sum(values):
    if lax.axis_size("tp") != 2:
        return lax.psum(values, "tp")
    return values + lax.ppermute(values, "tp", [(0, 1), (1, 0)])


def tp_scatter_sum(partial):
    if lax.axis_size("tp") != 2:
        pieces = lax.all_to_all(
            partial.reshape(partial.shape[0], lax.axis_size("tp"), -1), "tp", 1, 1
        )
        return jnp.sum(pieces.astype(jnp.float32), axis=1)
    half = partial.shape[1] // 2
    low = lax.axis_index("tp") == 0
    keep = jnp.where(low, partial[:, :half], partial[:, half:])
    send = jnp.where(low, partial[:, half:], partial[:, :half])
    got = lax.ppermute(send, "tp", [(0, 1), (1, 0)])
    return keep.astype(jnp.float32) + got.astype(jnp.float32)


def product_rows(left, groups, columns=slice(None)):
    result = 0.0
    for pieces, blocks in zip(left, groups):
        for piece, block in zip(pieces, blocks):
            result = result + jnp.dot(
                piece, block[:, columns], preferred_element_type=jnp.float32
            )
    return result


def product_columns(left, groups, place, core, columns=None):
    terms = []
    for blocks in groups:
        pair = []
        for block in blocks:
            if columns is None:
                dims, right = (((1,), (0,)), ((), ())), block
            else:
                dims, right = (((1,), (1,)), ((), ())), block[:, columns]
            term = lax.dot_general(left, right, dims, preferred_element_type=jnp.float32)
            pair.append(term.astype(jnp.bfloat16))
        terms.append(pair)
    return from_ring(terms, place, core)


def body(
    tokens,
    mix_gain,
    query_weight,
    key_weight,
    value_weight,
    output_gate_weight,
    out_weight,
    head_rates,
    block_scale,
    ffn_gain,
    ff_gate,
    ff_up,
    ff_down,
    final_gain,
):
    rows = tokens.shape[0]
    heads_here = head_rates.shape[0]
    size = lax.axis_size("fs")
    place, core = ring_place(size)
    reach = (size // 2 - 1) // 2
    positions = jnp.arange(rows, dtype=jnp.int32) % SEQ_LEN

    bundle = jnp.concatenate(
        [query_weight, key_weight, value_weight, output_gate_weight, out_weight.T], axis=1
    )
    hops, proj = circulate(bundle, 0)
    last = (hops[-reach], hops[reach])
    gate_hops, gates = circulate(ff_gate, 0, ((), last))
    _, ups = circulate(ff_up, 0, ((hops[1 - reach], hops[reach - 1]),))
    _, downs = circulate(ff_down, 1, ((gate_hops[-reach], gate_hops[reach]),))

    whole = tp_gather(tokens, 1)
    gains = tp_gather(jnp.stack([mix_gain, ffn_gain]), 1)
    normed = rms_norm(whole.astype(jnp.float32), gains[0]).astype(jnp.bfloat16)
    width = bundle.shape[1] - out_weight.shape[0]
    projected = product_rows(to_ring(normed, place, core), proj, slice(0, width))
    ends = [query_weight.shape[1], key_weight.shape[1], value_weight.shape[1]]
    qproj, kproj, vproj, gproj = jnp.split(
        projected, [ends[0], ends[0] + ends[1], sum(ends)], axis=1
    )
    query = rotate(qproj.reshape(rows, heads_here, DK), positions).astype(jnp.bfloat16)
    key = (rotate(kproj.reshape(rows, heads_here, DK), positions) * DK ** (-0.5)).astype(
        jnp.bfloat16
    )
    value = vproj.astype(jnp.bfloat16).reshape(rows, heads_here, DV)
    normret = retain(query, key, value, head_rates, block_scale)
    gated = (normret * jax.nn.silu(gproj)).astype(jnp.bfloat16)
    mix = tp_scatter_sum(product_columns(gated, proj, place, core, slice(width, None)))
    resid = (tokens.astype(jnp.float32) + mix).astype(jnp.bfloat16)
    whole2 = tp_gather(resid, 1)
    normed2 = to_ring(
        rms_norm(whole2.astype(jnp.float32), gains[1]).astype(jnp.bfloat16), place, core
    )
    gate_part = product_rows(normed2, gates)
    up_part = product_rows(normed2, ups)
    hidden = (jax.nn.silu(gate_part) * up_part).astype(jnp.bfloat16)
    ffn = tp_scatter_sum(product_columns(hidden, downs, place, core))
    total = resid.astype(jnp.float32) + ffn
    squares = tp_sum(jnp.sum(total * total, axis=-1))[:, None]
    scale = lax.rsqrt(squares / D + EPS)
    return (total * scale * final_gain.astype(jnp.float32)).astype(jnp.bfloat16)


def solution(mesh):
    return jax.shard_map(
        body,
        mesh=mesh,
        in_specs=(
            P("fs", "tp"),
            P("tp"),
            P("fs", "tp"),
            P("fs", "tp"),
            P("fs", "tp"),
            P("fs", "tp"),
            P("tp", "fs"),
            P("tp"),
            P("fs"),
            P("tp"),
            P("fs", "tp"),
            P("fs", "tp"),
            P("tp", "fs"),
            P("tp"),
        ),
        out_specs=P("fs", "tp"),
        check_vma=False,
    )
```

```python
import jax
import jax.numpy as jnp
from jax import lax
from jax.sharding import PartitionSpec as P

D = 2048
DK = 64
DV = 128
BLK = 128
SEQ_LEN = 256


EPS = 1e-06
THETA = 10000.0


def rms_norm(values, gain):
    scale = lax.rsqrt(jnp.mean(values * values, axis=-1, keepdims=True) + EPS)
    return values * scale * gain.astype(jnp.float32)


def rotate(values, positions):
    half = values.shape[-1] // 2
    inverse = THETA ** (-jnp.arange(half, dtype=jnp.float32) / half)
    angle = positions.astype(jnp.float32)[:, None] * inverse
    cosine = jnp.cos(angle)[:, None, :]
    sine = jnp.sin(angle)[:, None, :]
    first = values[..., :half]
    second = values[..., half:]
    return jnp.concatenate(
        [first * cosine - second * sine, second * cosine + first * sine], axis=-1
    )


def retain(query, key, value, rates, scales):
    rows, heads_here, width_k = query.shape
    width_v = value.shape[-1]
    nblk = rows // BLK
    hi = lax.Precision.HIGHEST
    qblk = query.astype(jnp.float32).reshape(nblk, BLK, heads_here, width_k)
    kblk = key.astype(jnp.float32).reshape(nblk, BLK, heads_here, width_k)
    vblk = value.astype(jnp.float32).reshape(nblk, BLK, heads_here, width_v)
    logdec = -rates[None, :] * scales[:, None]
    steps = jnp.arange(BLK, dtype=jnp.float32)
    offset = steps[:, None] - steps[None, :]
    causal = offset >= 0
    inside = jnp.where(
        causal[None, None],
        jnp.exp(logdec[:, :, None, None] * jnp.where(causal, offset, 0.0)[None, None]),
        0.0,
    )
    scores = jnp.einsum("nchd,nmhd->nhcm", qblk, kblk, precision=hi) * inside
    inner = jnp.einsum("nhcm,nmhe->nche", scores, vblk, precision=hi)
    zeta = jnp.exp(logdec[:, :, None] * (BLK - 1.0 - steps)[None, None, :])
    kv_block = jnp.einsum(
        "nchd,nche->nhde", kblk * jnp.transpose(zeta, (0, 2, 1))[..., None], vblk, precision=hi
    )
    hold = jnp.exp(logdec * BLK)
    per_seq = SEQ_LEN // BLK
    fresh = (jnp.arange(nblk, dtype=jnp.int32) % per_seq == 0).astype(jnp.float32)

    def advance(state, inputs):
        kv_now, hold_now, fresh_now = inputs
        before = state * (1.0 - fresh_now)
        return (before * hold_now[:, None, None] + kv_now, before)

    start = jnp.zeros((heads_here, width_k, width_v), jnp.float32)
    _, before = lax.scan(advance, start, (kv_block, hold, fresh), unroll=True)
    xi = jnp.exp(logdec[:, :, None] * (steps + 1.0)[None, None, :])
    cross = jnp.einsum(
        "nchd,nhde->nche", qblk * jnp.transpose(xi, (0, 2, 1))[..., None], before, precision=hi
    )
    total = inner + cross
    total = total * lax.rsqrt(jnp.mean(total * total, axis=-1, keepdims=True) + EPS)
    return total.reshape(rows, heads_here * width_v)


def chip_ring(size):
    chips = size // 2
    return list(range(0, chips, 2)) + list(range(1, chips, 2))[::-1]


def ring_place(size):
    ring = chip_ring(size)
    me = lax.axis_index("fs")
    chip = me // 2
    place = jnp.zeros((), jnp.int32)
    for index, member in enumerate(ring):
        place = jnp.where(chip == member, index, place)
    return place, me % 2


def after(value, *others):
    return lax.optimization_barrier((value,) + tuple(others))[0]


def circulate(block, axis, gates=()):
    size = lax.axis_size("fs")
    ring = chip_ring(size)
    chips = len(ring)
    onward = [
        (2 * ring[i] + core, 2 * ring[(i + 1) % chips] + core)
        for i in range(chips)
        for core in range(2)
    ]
    back = [(target, source) for source, target in onward]
    swap = [(i, i ^ 1) for i in range(size)]
    held = {0: block}
    reach = (chips - 1) // 2
    down = up = block
    for step in range(1, reach + 1):
        if len(gates) >= step and gates[step - 1]:
            down = after(down, *gates[step - 1])
            up = after(up, *gates[step - 1])
        down = lax.ppermute(down, "fs", onward)
        up = lax.ppermute(up, "fs", back)
        held[-step] = down
        held[step] = up
    if chips % 2 == 0 and chips > 1:
        cut = 1 - axis
        half = block.shape[cut] // 2
        if len(gates) > reach and gates[reach]:
            down = after(down, *gates[reach])
            up = after(up, *gates[reach])
        first = lax.ppermute(lax.slice_in_dim(down, 0, half, axis=cut), "fs", onward)
        second = lax.ppermute(lax.slice_in_dim(up, half, None, axis=cut), "fs", back)
        held[reach + 1] = jnp.concatenate([first, second], axis=cut)
    groups = []
    for offsets in order_of(size):
        own = jnp.concatenate([held[o] for o in offsets], axis=axis)
        groups.append((own, lax.ppermute(own, "fs", swap)))
    return held, groups


def order_of(size):
    chips = size // 2
    reach = (chips - 1) // 2
    groups = [list(range(-reach, reach + 1))]
    if chips > 1 and chips % 2 == 0:
        groups.append([reach + 1])
    return groups


def lane_of(values, lane, wide):
    count = values.shape[1] // (2 * wide)
    return [values[:, (2 * c + lane) * wide : (2 * c + lane + 1) * wide] for c in range(count)]


def to_ring(values, place, core):
    size = lax.axis_size("fs")
    wide = values.shape[1] // size
    ring = chip_ring(size)
    chips = len(ring)
    groups = order_of(size)
    start = (place + groups[0][0] + chips) % chips
    lanes = []
    for lane in range(2):
        pieces = lane_of(values, lane, wide)
        ringed = jnp.concatenate([pieces[c] for c in ring] * 2, axis=1)
        lanes.append(lax.dynamic_slice_in_dim(ringed, start * wide, chips * wide, axis=1))
    own = jnp.where(core == 0, lanes[0], lanes[1])
    other = jnp.where(core == 0, lanes[1], lanes[0])
    result, edge = [], 0
    for offsets in groups:
        end = edge + len(offsets) * wide
        result.append((own[:, edge:end], other[:, edge:end]))
        edge = end
    return result


def from_ring(groups, place, core):
    size = lax.axis_size("fs")
    ring = chip_ring(size)
    chips = len(ring)
    own = jnp.concatenate([own for own, _ in groups], axis=1)
    other = jnp.concatenate([other for _, other in groups], axis=1)
    wide = own.shape[1] // chips
    start = (2 * chips - place - order_of(size)[0][0]) % chips
    lanes = []
    for lane in range(2):
        straight = jnp.where(core == lane, own, other)
        doubled = jnp.concatenate([straight, straight], axis=1)
        lanes.append(lax.dynamic_slice_in_dim(doubled, start * wide, chips * wide, axis=1))
    spot = {c: i for i, c in enumerate(ring)}
    return jnp.concatenate(
        [
            lanes[lane][:, spot[c] * wide : (spot[c] + 1) * wide]
            for c in range(chips)
            for lane in range(2)
        ],
        axis=1,
    )


def tp_gather(values, axis):
    if lax.axis_size("tp") != 2:
        return lax.all_gather(values, "tp", axis=axis, tiled=True)
    other = lax.ppermute(values, "tp", [(0, 1), (1, 0)])
    mine = lax.axis_index("tp") == 0
    return jnp.concatenate(
        [jnp.where(mine, values, other), jnp.where(mine, other, values)], axis=axis
    )


def tp_sum(values):
    if lax.axis_size("tp") != 2:
        return lax.psum(values, "tp")
    return values + lax.ppermute(values, "tp", [(0, 1), (1, 0)])


def tp_scatter_sum(partial):
    if lax.axis_size("tp") != 2:
        pieces = lax.all_to_all(
            partial.reshape(partial.shape[0], lax.axis_size("tp"), -1), "tp", 1, 1
        )
        return jnp.sum(pieces.astype(jnp.float32), axis=1)
    half = partial.shape[1] // 2
    low = lax.axis_index("tp") == 0
    keep = jnp.where(low, partial[:, :half], partial[:, half:])
    send = jnp.where(low, partial[:, half:], partial[:, :half])
    got = lax.ppermute(send, "tp", [(0, 1), (1, 0)])
    return keep.astype(jnp.float32) + got.astype(jnp.float32)


def product_rows(left, groups, columns=slice(None), result=0.0):
    for pieces, blocks in zip(left, groups):
        for piece, block in zip(pieces, blocks):
            result = result + jnp.dot(
                piece, block[:, columns], preferred_element_type=jnp.float32
            )
    return result


def product_columns(left, groups, place, core, columns=None):
    terms = []
    for blocks in groups:
        pair = []
        for block in blocks:
            if columns is None:
                dims, right = (((1,), (0,)), ((), ())), block
            else:
                dims, right = (((1,), (1,)), ((), ())), block[:, columns]
            term = lax.dot_general(left, right, dims, preferred_element_type=jnp.float32)
            pair.append(term.astype(jnp.bfloat16))
        terms.append(pair)
    return from_ring(terms, place, core)


def body(
    tokens,
    mix_gain,
    query_weight,
    key_weight,
    value_weight,
    output_gate_weight,
    out_weight,
    head_rates,
    block_scale,
    ffn_gain,
    ff_gate,
    ff_up,
    ff_down,
    final_gain,
):
    rows = tokens.shape[0]
    heads_here = head_rates.shape[0]
    size = lax.axis_size("fs")
    place, core = ring_place(size)
    reach = (size // 2 - 1) // 2
    positions = jnp.arange(rows, dtype=jnp.int32) % SEQ_LEN

    bundle = jnp.concatenate(
        [query_weight, key_weight, value_weight, output_gate_weight, out_weight.T], axis=1
    )
    hops, proj = circulate(bundle, 0)
    last = (hops[-reach], hops[reach])

    whole = tp_gather(tokens, 1)
    gains = tp_gather(jnp.stack([mix_gain, ffn_gain]), 1)
    normed = rms_norm(whole.astype(jnp.float32), gains[0]).astype(jnp.bfloat16)
    width = bundle.shape[1] - out_weight.shape[0]
    projected = product_rows(to_ring(normed, place, core), proj, slice(0, width))
    ends = [query_weight.shape[1], key_weight.shape[1], value_weight.shape[1]]
    qproj, kproj, vproj, gproj = jnp.split(
        projected, [ends[0], ends[0] + ends[1], sum(ends)], axis=1
    )
    query = rotate(qproj.reshape(rows, heads_here, DK), positions).astype(jnp.bfloat16)
    key = (rotate(kproj.reshape(rows, heads_here, DK), positions) * DK ** (-0.5)).astype(
        jnp.bfloat16
    )
    value = vproj.astype(jnp.bfloat16).reshape(rows, heads_here, DV)
    normret = retain(query, key, value, head_rates, block_scale)
    gated = (normret * jax.nn.silu(gproj)).astype(jnp.bfloat16)
    opposite = tuple(hops[o] for o in order_of(size)[-1])
    gate_hops, gates = circulate(ff_gate, 0, ((), opposite, (projected,)))
    up_hops, ups = circulate(ff_up, 0, (last, (), (gated,)))
    mix = tp_scatter_sum(product_columns(gated, proj, place, core, slice(width, None)))
    resid = (tokens.astype(jnp.float32) + mix).astype(jnp.bfloat16)
    whole2 = tp_gather(resid, 1)
    normed2 = to_ring(
        rms_norm(whole2.astype(jnp.float32), gains[1]).astype(jnp.bfloat16), place, core
    )
    gate_part = product_rows(normed2[:1], gates[:1])
    up_part = product_rows(normed2[:1], ups[:1])
    early_parts = (gate_part, up_part)
    gate_part = product_rows(normed2[1:], gates[1:], result=gate_part)
    up_part = product_rows(normed2[1:], ups[1:], result=up_part)
    hidden = (jax.nn.silu(gate_part) * up_part).astype(jnp.bfloat16)
    near = (gate_hops[-reach], gate_hops[reach])
    _, downs = circulate(ff_down, 1, (near, (normed2[0][0],), early_parts, (hidden,)))
    ffn = tp_scatter_sum(product_columns(hidden, downs, place, core))
    total = resid.astype(jnp.float32) + ffn
    squares = tp_sum(jnp.sum(total * total, axis=-1))[:, None]
    scale = lax.rsqrt(squares / D + EPS)
    return (total * scale * final_gain.astype(jnp.float32)).astype(jnp.bfloat16)


def solution(mesh):
    return jax.shard_map(
        body,
        mesh=mesh,
        in_specs=(
            P("fs", "tp"),
            P("tp"),
            P("fs", "tp"),
            P("fs", "tp"),
            P("fs", "tp"),
            P("fs", "tp"),
            P("tp", "fs"),
            P("tp"),
            P("fs"),
            P("tp"),
            P("fs", "tp"),
            P("fs", "tp"),
            P("tp", "fs"),
            P("tp"),
        ),
        out_specs=P("fs", "tp"),
        check_vma=False,
    )
```

```python
import jax
import jax.numpy as jnp
from jax import lax
from jax.sharding import PartitionSpec as P

D = 2048
DK = 64
DV = 128
BLK = 128
SEQ_LEN = 256


EPS = 1e-06
THETA = 10000.0


def rms_norm(values, gain):
    scale = lax.rsqrt(jnp.mean(values * values, axis=-1, keepdims=True) + EPS)
    return values * scale * gain.astype(jnp.float32)


def rotate(values, positions):
    half = values.shape[-1] // 2
    inverse = THETA ** (-jnp.arange(half, dtype=jnp.float32) / half)
    angle = positions.astype(jnp.float32)[:, None] * inverse
    cosine = jnp.cos(angle)[:, None, :]
    sine = jnp.sin(angle)[:, None, :]
    first = values[..., :half]
    second = values[..., half:]
    return jnp.concatenate(
        [first * cosine - second * sine, second * cosine + first * sine], axis=-1
    )


def retain(query, key, value, rates, scales):
    rows, heads_here, width_k = query.shape
    width_v = value.shape[-1]
    nblk = rows // BLK
    hi = lax.Precision.HIGHEST
    qblk = query.astype(jnp.float32).reshape(nblk, BLK, heads_here, width_k)
    kblk = key.astype(jnp.float32).reshape(nblk, BLK, heads_here, width_k)
    vblk = value.astype(jnp.float32).reshape(nblk, BLK, heads_here, width_v)
    logdec = -rates[None, :] * scales[:, None]
    steps = jnp.arange(BLK, dtype=jnp.float32)
    offset = steps[:, None] - steps[None, :]
    causal = offset >= 0
    inside = jnp.where(
        causal[None, None],
        jnp.exp(logdec[:, :, None, None] * jnp.where(causal, offset, 0.0)[None, None]),
        0.0,
    )
    scores = jnp.einsum("nchd,nmhd->nhcm", qblk, kblk, precision=hi) * inside
    inner = jnp.einsum("nhcm,nmhe->nche", scores, vblk, precision=hi)
    zeta = jnp.exp(logdec[:, :, None] * (BLK - 1.0 - steps)[None, None, :])
    kv_block = jnp.einsum(
        "nchd,nche->nhde", kblk * jnp.transpose(zeta, (0, 2, 1))[..., None], vblk, precision=hi
    )
    hold = jnp.exp(logdec * BLK)
    per_seq = SEQ_LEN // BLK
    fresh = (jnp.arange(nblk, dtype=jnp.int32) % per_seq == 0).astype(jnp.float32)

    def advance(state, inputs):
        kv_now, hold_now, fresh_now = inputs
        before = state * (1.0 - fresh_now)
        return (before * hold_now[:, None, None] + kv_now, before)

    start = jnp.zeros((heads_here, width_k, width_v), jnp.float32)
    _, before = lax.scan(advance, start, (kv_block, hold, fresh), unroll=True)
    xi = jnp.exp(logdec[:, :, None] * (steps + 1.0)[None, None, :])
    cross = jnp.einsum(
        "nchd,nhde->nche", qblk * jnp.transpose(xi, (0, 2, 1))[..., None], before, precision=hi
    )
    total = inner + cross
    total = total * lax.rsqrt(jnp.mean(total * total, axis=-1, keepdims=True) + EPS)
    return total.reshape(rows, heads_here * width_v)


def chip_ring(size):
    chips = size // 2
    return list(range(0, chips, 2)) + list(range(1, chips, 2))[::-1]


def ring_place(size):
    ring = chip_ring(size)
    me = lax.axis_index("fs")
    chip = me // 2
    place = jnp.zeros((), jnp.int32)
    for index, member in enumerate(ring):
        place = jnp.where(chip == member, index, place)
    return place, me % 2


def after(value, *others):
    return lax.optimization_barrier((value,) + tuple(others))[0]


def circulate(block, axis, gates=()):
    size = lax.axis_size("fs")
    ring = chip_ring(size)
    chips = len(ring)
    onward = [
        (2 * ring[i] + core, 2 * ring[(i + 1) % chips] + core)
        for i in range(chips)
        for core in range(2)
    ]
    back = [(target, source) for source, target in onward]
    swap = [(i, i ^ 1) for i in range(size)]
    held = {0: block}
    reach = (chips - 1) // 2
    down = up = block
    for step in range(1, reach + 1):
        if len(gates) >= step and gates[step - 1]:
            down = after(down, *gates[step - 1])
            up = after(up, *gates[step - 1])
        down = lax.ppermute(down, "fs", onward)
        up = lax.ppermute(up, "fs", back)
        held[-step] = down
        held[step] = up
    if chips % 2 == 0 and chips > 1:
        cut = 1 - axis
        half = block.shape[cut] // 2
        if len(gates) > reach and gates[reach]:
            down = after(down, *gates[reach])
            up = after(up, *gates[reach])
        first = lax.ppermute(lax.slice_in_dim(down, 0, half, axis=cut), "fs", onward)
        second = lax.ppermute(lax.slice_in_dim(up, half, None, axis=cut), "fs", back)
        held[reach + 1] = jnp.concatenate([first, second], axis=cut)
    groups = []
    for offsets in order_of(size):
        own = jnp.concatenate([held[o] for o in offsets], axis=axis)
        groups.append((own, lax.ppermute(own, "fs", swap)))
    return held, groups


def order_of(size):
    chips = size // 2
    reach = (chips - 1) // 2
    groups = [list(range(-reach, reach + 1))]
    if chips > 1 and chips % 2 == 0:
        groups.append([reach + 1])
    return groups


def lane_of(values, lane, wide):
    count = values.shape[1] // (2 * wide)
    return [values[:, (2 * c + lane) * wide : (2 * c + lane + 1) * wide] for c in range(count)]


def to_ring(values, place, core):
    size = lax.axis_size("fs")
    wide = values.shape[1] // size
    ring = chip_ring(size)
    chips = len(ring)
    groups = order_of(size)
    start = (place + groups[0][0] + chips) % chips
    lanes = []
    for lane in range(2):
        pieces = lane_of(values, lane, wide)
        ringed = jnp.concatenate([pieces[c] for c in ring] * 2, axis=1)
        lanes.append(lax.dynamic_slice_in_dim(ringed, start * wide, chips * wide, axis=1))
    own = jnp.where(core == 0, lanes[0], lanes[1])
    other = jnp.where(core == 0, lanes[1], lanes[0])
    result, edge = [], 0
    for offsets in groups:
        end = edge + len(offsets) * wide
        result.append((own[:, edge:end], other[:, edge:end]))
        edge = end
    return result


def from_ring(groups, place, core):
    size = lax.axis_size("fs")
    ring = chip_ring(size)
    chips = len(ring)
    own = jnp.concatenate([own for own, _ in groups], axis=1)
    other = jnp.concatenate([other for _, other in groups], axis=1)
    wide = own.shape[1] // chips
    start = (2 * chips - place - order_of(size)[0][0]) % chips
    lanes = []
    for lane in range(2):
        straight = jnp.where(core == lane, own, other)
        doubled = jnp.concatenate([straight, straight], axis=1)
        lanes.append(lax.dynamic_slice_in_dim(doubled, start * wide, chips * wide, axis=1))
    spot = {c: i for i, c in enumerate(ring)}
    return jnp.concatenate(
        [
            lanes[lane][:, spot[c] * wide : (spot[c] + 1) * wide]
            for c in range(chips)
            for lane in range(2)
        ],
        axis=1,
    )


def tp_gather(values, axis):
    if lax.axis_size("tp") != 2:
        return lax.all_gather(values, "tp", axis=axis, tiled=True)
    other = lax.ppermute(values, "tp", [(0, 1), (1, 0)])
    mine = lax.axis_index("tp") == 0
    return jnp.concatenate(
        [jnp.where(mine, values, other), jnp.where(mine, other, values)], axis=axis
    )


def tp_sum(values):
    if lax.axis_size("tp") != 2:
        return lax.psum(values, "tp")
    return values + lax.ppermute(values, "tp", [(0, 1), (1, 0)])


def tp_scatter_sum(partial):
    if lax.axis_size("tp") != 2:
        pieces = lax.all_to_all(
            partial.reshape(partial.shape[0], lax.axis_size("tp"), -1), "tp", 1, 1
        )
        return jnp.sum(pieces.astype(jnp.float32), axis=1)
    half = partial.shape[1] // 2
    low = lax.axis_index("tp") == 0
    keep = jnp.where(low, partial[:, :half], partial[:, half:])
    send = jnp.where(low, partial[:, half:], partial[:, :half])
    got = lax.ppermute(send, "tp", [(0, 1), (1, 0)])
    return keep.astype(jnp.float32) + got.astype(jnp.float32)


def product_rows(left, groups, columns=slice(None), result=0.0):
    for pieces, blocks in zip(left, groups):
        for piece, block in zip(pieces, blocks):
            result = result + jnp.dot(
                piece, block[:, columns], preferred_element_type=jnp.float32
            )
    return result


def product_columns(left, groups, place, core, columns=None):
    terms = []
    for blocks in groups:
        pair = []
        for block in blocks:
            if columns is None:
                dims, right = (((1,), (0,)), ((), ())), block
            else:
                dims, right = (((1,), (1,)), ((), ())), block[:, columns]
            term = lax.dot_general(left, right, dims, preferred_element_type=jnp.float32)
            pair.append(term.astype(jnp.bfloat16))
        terms.append(pair)
    return from_ring(terms, place, core)


def body(
    tokens,
    mix_gain,
    query_weight,
    key_weight,
    value_weight,
    output_gate_weight,
    out_weight,
    head_rates,
    block_scale,
    ffn_gain,
    ff_gate,
    ff_up,
    ff_down,
    final_gain,
):
    rows = tokens.shape[0]
    heads_here = head_rates.shape[0]
    size = lax.axis_size("fs")
    place, core = ring_place(size)
    reach = (size // 2 - 1) // 2
    positions = jnp.arange(rows, dtype=jnp.int32) % SEQ_LEN

    bundle = jnp.concatenate(
        [query_weight, key_weight, value_weight, output_gate_weight, out_weight.T], axis=1
    )
    hops, proj = circulate(bundle, 0)
    last = (hops[-reach], hops[reach])

    whole = tp_gather(tokens, 1)
    gains = tp_gather(jnp.stack([mix_gain, ffn_gain]), 1)
    normed = rms_norm(whole.astype(jnp.float32), gains[0]).astype(jnp.bfloat16)
    width = bundle.shape[1] - out_weight.shape[0]
    projected = product_rows(to_ring(normed, place, core), proj, slice(0, width))
    ends = [query_weight.shape[1], key_weight.shape[1], value_weight.shape[1]]
    qproj, kproj, vproj, gproj = jnp.split(
        projected, [ends[0], ends[0] + ends[1], sum(ends)], axis=1
    )
    query = rotate(qproj.reshape(rows, heads_here, DK), positions).astype(jnp.bfloat16)
    key = (rotate(kproj.reshape(rows, heads_here, DK), positions) * DK ** (-0.5)).astype(
        jnp.bfloat16
    )
    value = vproj.astype(jnp.bfloat16).reshape(rows, heads_here, DV)
    normret = retain(query, key, value, head_rates, block_scale)
    gated = (normret * jax.nn.silu(gproj)).astype(jnp.bfloat16)
    opposite = tuple(hops[o] for o in order_of(size)[-1])
    gate_hops, gates = circulate(ff_gate, 0, ((), opposite, (projected,)))
    up_hops, ups = circulate(ff_up, 0, (last, (), (gated,)))
    mix = tp_scatter_sum(product_columns(gated, proj, place, core, slice(width, None)))
    resid = (tokens.astype(jnp.float32) + mix).astype(jnp.bfloat16)
    whole2 = tp_gather(resid, 1)
    normed2 = to_ring(
        rms_norm(whole2.astype(jnp.float32), gains[1]).astype(jnp.bfloat16), place, core
    )
    gate_part = product_rows(normed2[:1], gates[:1])
    up_part = product_rows(normed2[:1], ups[:1])
    early_parts = (gate_part, up_part)
    gate_part = product_rows(normed2[1:], gates[1:], result=gate_part)
    up_part = product_rows(normed2[1:], ups[1:], result=up_part)
    hidden = (jax.nn.silu(gate_part) * up_part).astype(jnp.bfloat16)
    near = (gate_hops[-reach], gate_hops[reach])
    far = order_of(size)[-1][-1]
    second = (normed2[0][0], up_hops[-reach], up_hops[reach])
    third = early_parts + (gate_hops[far], up_hops[far])
    _, downs = circulate(ff_down, 1, (near, second, third, (hidden,)))
    ffn = tp_scatter_sum(product_columns(hidden, downs, place, core))
    total = resid.astype(jnp.float32) + ffn
    squares = tp_sum(jnp.sum(total * total, axis=-1))[:, None]
    scale = lax.rsqrt(squares / D + EPS)
    return (total * scale * final_gain.astype(jnp.float32)).astype(jnp.bfloat16)


def solution(mesh):
    return jax.shard_map(
        body,
        mesh=mesh,
        in_specs=(
            P("fs", "tp"),
            P("tp"),
            P("fs", "tp"),
            P("fs", "tp"),
            P("fs", "tp"),
            P("fs", "tp"),
            P("tp", "fs"),
            P("tp"),
            P("fs"),
            P("tp"),
            P("fs", "tp"),
            P("fs", "tp"),
            P("tp", "fs"),
            P("tp"),
        ),
        out_specs=P("fs", "tp"),
        check_vma=False,
    )
```

```python
import jax
import jax.numpy as jnp
from jax import lax
from jax.sharding import PartitionSpec as P

D = 2048
DK = 64
DV = 128
BLK = 128
SEQ_LEN = 256


EPS = 1e-06
THETA = 10000.0


def rms_norm(values, gain):
    scale = lax.rsqrt(jnp.mean(values * values, axis=-1, keepdims=True) + EPS)
    return values * scale * gain.astype(jnp.float32)


def rotate(values, positions):
    half = values.shape[-1] // 2
    inverse = THETA ** (-jnp.arange(half, dtype=jnp.float32) / half)
    angle = positions.astype(jnp.float32)[:, None] * inverse
    cosine = jnp.cos(angle)[:, None, :]
    sine = jnp.sin(angle)[:, None, :]
    first = values[..., :half]
    second = values[..., half:]
    return jnp.concatenate(
        [first * cosine - second * sine, second * cosine + first * sine], axis=-1
    )


def retain(query, key, value, rates, scales):
    rows, heads_here, width_k = query.shape
    width_v = value.shape[-1]
    nblk = rows // BLK
    hi = lax.Precision.HIGHEST
    qblk = query.astype(jnp.float32).reshape(nblk, BLK, heads_here, width_k)
    kblk = key.astype(jnp.float32).reshape(nblk, BLK, heads_here, width_k)
    vblk = value.astype(jnp.float32).reshape(nblk, BLK, heads_here, width_v)
    logdec = -rates[None, :] * scales[:, None]
    steps = jnp.arange(BLK, dtype=jnp.float32)
    offset = steps[:, None] - steps[None, :]
    causal = offset >= 0
    inside = jnp.where(
        causal[None, None],
        jnp.exp(logdec[:, :, None, None] * jnp.where(causal, offset, 0.0)[None, None]),
        0.0,
    )
    scores = jnp.einsum("nchd,nmhd->nhcm", qblk, kblk, precision=hi) * inside
    inner = jnp.einsum("nhcm,nmhe->nche", scores, vblk, precision=hi)
    zeta = jnp.exp(logdec[:, :, None] * (BLK - 1.0 - steps)[None, None, :])
    kv_block = jnp.einsum(
        "nchd,nche->nhde", kblk * jnp.transpose(zeta, (0, 2, 1))[..., None], vblk, precision=hi
    )
    hold = jnp.exp(logdec * BLK)
    per_seq = SEQ_LEN // BLK
    fresh = (jnp.arange(nblk, dtype=jnp.int32) % per_seq == 0).astype(jnp.float32)

    def advance(state, inputs):
        kv_now, hold_now, fresh_now = inputs
        before = state * (1.0 - fresh_now)
        return (before * hold_now[:, None, None] + kv_now, before)

    start = jnp.zeros((heads_here, width_k, width_v), jnp.float32)
    _, before = lax.scan(advance, start, (kv_block, hold, fresh), unroll=True)
    xi = jnp.exp(logdec[:, :, None] * (steps + 1.0)[None, None, :])
    cross = jnp.einsum(
        "nchd,nhde->nche", qblk * jnp.transpose(xi, (0, 2, 1))[..., None], before, precision=hi
    )
    total = inner + cross
    total = total * lax.rsqrt(jnp.mean(total * total, axis=-1, keepdims=True) + EPS)
    return total.reshape(rows, heads_here * width_v)


def chip_ring(size):
    chips = size // 2
    return list(range(0, chips, 2)) + list(range(1, chips, 2))[::-1]


def ring_place(size):
    ring = chip_ring(size)
    me = lax.axis_index("fs")
    chip = me // 2
    place = jnp.zeros((), jnp.int32)
    for index, member in enumerate(ring):
        place = jnp.where(chip == member, index, place)
    return place, me % 2


def after(value, *others):
    return lax.optimization_barrier((value,) + tuple(others))[0]


def circulate(block, axis, gates=()):
    size = lax.axis_size("fs")
    ring = chip_ring(size)
    chips = len(ring)
    onward = [
        (2 * ring[i] + core, 2 * ring[(i + 1) % chips] + core)
        for i in range(chips)
        for core in range(2)
    ]
    back = [(target, source) for source, target in onward]
    swap = [(i, i ^ 1) for i in range(size)]
    held = {0: block}
    reach = (chips - 1) // 2
    down = up = block
    for step in range(1, reach + 1):
        if len(gates) >= step and gates[step - 1]:
            down = after(down, *gates[step - 1])
            up = after(up, *gates[step - 1])
        down = lax.ppermute(down, "fs", onward)
        up = lax.ppermute(up, "fs", back)
        held[-step] = down
        held[step] = up
    if chips % 2 == 0 and chips > 1:
        cut = 1 - axis
        half = block.shape[cut] // 2
        if len(gates) > reach and gates[reach]:
            down = after(down, *gates[reach])
            up = after(up, *gates[reach])
        first = lax.ppermute(lax.slice_in_dim(down, 0, half, axis=cut), "fs", onward)
        second = lax.ppermute(lax.slice_in_dim(up, half, None, axis=cut), "fs", back)
        held[reach + 1] = jnp.concatenate([first, second], axis=cut)
    groups = []
    for offsets in order_of(size):
        own = jnp.concatenate([held[o] for o in offsets], axis=axis)
        groups.append((own, lax.ppermute(own, "fs", swap)))
    return held, groups


def order_of(size):
    chips = size // 2
    reach = (chips - 1) // 2
    groups = [list(range(-reach, reach + 1))]
    if chips > 1 and chips % 2 == 0:
        groups.append([reach + 1])
    return groups


def lane_of(values, lane, wide):
    count = values.shape[1] // (2 * wide)
    return [values[:, (2 * c + lane) * wide : (2 * c + lane + 1) * wide] for c in range(count)]


def to_ring(values, place, core):
    size = lax.axis_size("fs")
    wide = values.shape[1] // size
    ring = chip_ring(size)
    chips = len(ring)
    groups = order_of(size)
    start = (place + groups[0][0] + chips) % chips
    lanes = []
    for lane in range(2):
        pieces = lane_of(values, lane, wide)
        ringed = jnp.concatenate([pieces[c] for c in ring] * 2, axis=1)
        lanes.append(lax.dynamic_slice_in_dim(ringed, start * wide, chips * wide, axis=1))
    own = jnp.where(core == 0, lanes[0], lanes[1])
    other = jnp.where(core == 0, lanes[1], lanes[0])
    result, edge = [], 0
    for offsets in groups:
        end = edge + len(offsets) * wide
        result.append((own[:, edge:end], other[:, edge:end]))
        edge = end
    return result


def from_ring(groups, place, core):
    size = lax.axis_size("fs")
    ring = chip_ring(size)
    chips = len(ring)
    own = jnp.concatenate([own for own, _ in groups], axis=1)
    other = jnp.concatenate([other for _, other in groups], axis=1)
    wide = own.shape[1] // chips
    start = (2 * chips - place - order_of(size)[0][0]) % chips
    lanes = []
    for lane in range(2):
        straight = jnp.where(core == lane, own, other)
        doubled = jnp.concatenate([straight, straight], axis=1)
        lanes.append(lax.dynamic_slice_in_dim(doubled, start * wide, chips * wide, axis=1))
    spot = {c: i for i, c in enumerate(ring)}
    return jnp.concatenate(
        [
            lanes[lane][:, spot[c] * wide : (spot[c] + 1) * wide]
            for c in range(chips)
            for lane in range(2)
        ],
        axis=1,
    )


def tp_gather(values, axis):
    if lax.axis_size("tp") != 2:
        return lax.all_gather(values, "tp", axis=axis, tiled=True)
    other = lax.ppermute(values, "tp", [(0, 1), (1, 0)])
    mine = lax.axis_index("tp") == 0
    return jnp.concatenate(
        [jnp.where(mine, values, other), jnp.where(mine, other, values)], axis=axis
    )


def tp_sum(values):
    if lax.axis_size("tp") != 2:
        return lax.psum(values, "tp")
    return values + lax.ppermute(values, "tp", [(0, 1), (1, 0)])


def tp_scatter_sum(partial):
    if lax.axis_size("tp") != 2:
        pieces = lax.all_to_all(
            partial.reshape(partial.shape[0], lax.axis_size("tp"), -1), "tp", 1, 1
        )
        return jnp.sum(pieces.astype(jnp.float32), axis=1)
    half = partial.shape[1] // 2
    low = lax.axis_index("tp") == 0
    keep = jnp.where(low, partial[:, :half], partial[:, half:])
    send = jnp.where(low, partial[:, half:], partial[:, :half])
    got = lax.ppermute(send, "tp", [(0, 1), (1, 0)])
    return keep.astype(jnp.float32) + got.astype(jnp.float32)


def product_rows(left, groups, columns=slice(None), result=0.0):
    for pieces, blocks in zip(left, groups):
        for piece, block in zip(pieces, blocks):
            result = result + jnp.dot(
                piece, block[:, columns], preferred_element_type=jnp.float32
            )
    return result


def product_columns(left, groups, place, core, columns=None):
    terms = []
    for blocks in groups:
        pair = []
        for block in blocks:
            if columns is None:
                dims, right = (((1,), (0,)), ((), ())), block
            else:
                dims, right = (((1,), (1,)), ((), ())), block[:, columns]
            term = lax.dot_general(left, right, dims, preferred_element_type=jnp.float32)
            pair.append(term.astype(jnp.bfloat16))
        terms.append(pair)
    return from_ring(terms, place, core)


def body(
    tokens,
    mix_gain,
    query_weight,
    key_weight,
    value_weight,
    output_gate_weight,
    out_weight,
    head_rates,
    block_scale,
    ffn_gain,
    ff_gate,
    ff_up,
    ff_down,
    final_gain,
):
    rows = tokens.shape[0]
    heads_here = head_rates.shape[0]
    size = lax.axis_size("fs")
    place, core = ring_place(size)
    reach = (size // 2 - 1) // 2
    positions = jnp.arange(rows, dtype=jnp.int32) % SEQ_LEN

    bundle = jnp.concatenate(
        [query_weight, key_weight, value_weight, output_gate_weight, out_weight.T], axis=1
    )
    hops, proj = circulate(bundle, 0)
    last = (hops[-reach], hops[reach])

    whole = tp_gather(tokens, 1)
    gains = tp_gather(jnp.stack([mix_gain, ffn_gain]), 1)
    normed = rms_norm(whole.astype(jnp.float32), gains[0]).astype(jnp.bfloat16)
    width = bundle.shape[1] - out_weight.shape[0]
    projected = product_rows(to_ring(normed, place, core), proj, slice(0, width))
    ends = [query_weight.shape[1], key_weight.shape[1], value_weight.shape[1]]
    qproj, kproj, vproj, gproj = jnp.split(
        projected, [ends[0], ends[0] + ends[1], sum(ends)], axis=1
    )
    query = rotate(qproj.reshape(rows, heads_here, DK), positions).astype(jnp.bfloat16)
    key = (rotate(kproj.reshape(rows, heads_here, DK), positions) * DK ** (-0.5)).astype(
        jnp.bfloat16
    )
    value = vproj.astype(jnp.bfloat16).reshape(rows, heads_here, DV)
    normret = retain(query, key, value, head_rates, block_scale)
    gated = (normret * jax.nn.silu(gproj)).astype(jnp.bfloat16)
    opposite = tuple(hops[o] for o in order_of(size)[-1])
    gate_hops, gates = circulate(ff_gate, 0, ((), opposite, (projected,)))
    up_hops, ups = circulate(ff_up, 0, (last, (), (gated,)))
    mix = tp_scatter_sum(product_columns(gated, proj, place, core, slice(width, None)))
    resid = (tokens.astype(jnp.float32) + mix).astype(jnp.bfloat16)
    whole2 = tp_gather(resid, 1)
    normed2 = to_ring(
        rms_norm(whole2.astype(jnp.float32), gains[1]).astype(jnp.bfloat16), place, core
    )
    gate_part = product_rows(normed2[:1], gates[:1])
    up_part = product_rows(normed2[:1], ups[:1])
    early_parts = (gate_part, up_part)
    gate_part = product_rows(normed2[1:], gates[1:], result=gate_part)
    up_part = product_rows(normed2[1:], ups[1:], result=up_part)
    hidden = (jax.nn.silu(gate_part) * up_part).astype(jnp.bfloat16)
    near = (gate_hops[-reach], gate_hops[reach])
    far = order_of(size)[-1][-1]
    second = (normed2[0][0], up_hops[-reach], up_hops[reach])
    third = early_parts + (gate_hops[far], up_hops[far])
    _, downs = circulate(ff_down, 1, (near, second, third))
    ffn = tp_scatter_sum(product_columns(hidden, downs, place, core))
    total = resid.astype(jnp.float32) + ffn
    squares = tp_sum(jnp.sum(total * total, axis=-1))[:, None]
    scale = lax.rsqrt(squares / D + EPS)
    return (total * scale * final_gain.astype(jnp.float32)).astype(jnp.bfloat16)


def solution(mesh):
    return jax.shard_map(
        body,
        mesh=mesh,
        in_specs=(
            P("fs", "tp"),
            P("tp"),
            P("fs", "tp"),
            P("fs", "tp"),
            P("fs", "tp"),
            P("fs", "tp"),
            P("tp", "fs"),
            P("tp"),
            P("fs"),
            P("tp"),
            P("fs", "tp"),
            P("fs", "tp"),
            P("tp", "fs"),
            P("tp"),
        ),
        out_specs=P("fs", "tp"),
        check_vma=False,
    )
```
